32 devices in a mesh: sp: 16 (over z, y, x), tp: 2 (over core).
Axes of the slice: x: 2, y: 2, z: 4, core: 2. Of those that a mesh axis runs over, the one named last changes fastest.
Arguments:
- tokens: bfloat16 [2048, 2048], P('sp'), may hold values from -6 to 6
- input_norm_gain: float32 [2048], replicated, may hold values from 0.1 to 1.9
- delta_query_weight: bfloat16 [2048, 1024], P('sp', 'tp'), may hold values from -0.125 to 0.125
- delta_key_weight: bfloat16 [2048, 1024], P('sp', 'tp'), may hold values from -0.125 to 0.125
- delta_value_weight: bfloat16 [2048, 1024], P('sp', 'tp'), may hold values from -0.125 to 0.125
- gate_weight: bfloat16 [2048, 4, 16], replicated, may hold values from -0.125 to 0.125
- head_decay_params: float32 [2, 16], P(None, 'tp'), may hold values from -20 to 1
- log_decay_increments: float32 [16, 2048], P('tp', 'sp'), may hold values from -2 to 0
- starting_state: float32 [2, 16, 64, 64], P(None, 'tp'), may hold values from -1.5 to 1.5
- delta_norm_gain: float32 [64], replicated, may hold values from 0.1 to 1.9
- attention_query_weight: bfloat16 [2048, 1024], P('sp', 'tp'), may hold values from -1 to 1
- attention_key_weight: bfloat16 [2048, 512], P('sp', 'tp'), may hold values from -64 to 64
- attention_value_weight: bfloat16 [2048, 512], P('sp', 'tp'), may hold values from -0.125 to 0.125
- sink: float32 [16], P('tp'), may hold values from -1 to 3
- delta_output_weight: bfloat16 [1024, 2048], P('tp'), may hold values from -0.125 to 0.125
- attention_output_weight: bfloat16 [1024, 2048], P('tp'), may hold values from -0.125 to 0.125
Outputs:
- mixed: bfloat16 [2048, 2048], P(('sp', 'tp'))
The draws below stay inside these ranges and needn't reach their ends.
All inputs are finite; a program needn't handle non-finite values.
Results may differ from the reference program's by a relative error of at most 0.018.
Values may be sent and summed in bfloat16 or wider, within the bound.
A program may use at most 128 MiB of HBM per device.

```python
import math
import jax
import jax.numpy as jnp
from jax import lax

D = 2048
DELTA_HEADS = 16
ATTN_HEADS = 16
KV_HEADS = 8
HEAD = 64
WINDOW = 128
BLOCK = 64
TOK_DEV = 128
TOKENS = 2048
N_TP = 2


def draw_tokens(key, part):
    baseline_value = jax.random.normal(jax.random.fold_in(key, 101), (TOKENS, D), jnp.float32)
    return jnp.clip(baseline_value, -6.0, 6.0).astype(jnp.bfloat16)


def attention_pair(key):
    query_rows = jax.random.normal(jax.random.fold_in(key, 201), (D, ATTN_HEADS * HEAD), jnp.float32) * D ** (-0.5)
    keys = jax.random.normal(jax.random.fold_in(key, 202), (D, KV_HEADS * HEAD), jnp.float32) * D ** (-0.5)
    return (jnp.clip(query_rows, -1.0, 1.0), jnp.clip(keys, -64.0, 64.0))


def draw_attention_query_weight(key, part):
    return attention_pair(key)[0].astype(jnp.bfloat16)


def draw_attention_key_weight(key, part):
    return attention_pair(key)[1].astype(jnp.bfloat16)


def draw_head_decay_params(key, part):
    order = jax.random.permutation(jax.random.fold_in(key, 301), DELTA_HEADS)
    fast_count = DELTA_HEADS // 2
    fast = order < fast_count
    jitter = jax.random.uniform(jax.random.fold_in(key, 302), (2, DELTA_HEADS), jnp.float32, -0.3, 0.3)
    decay_rate = jnp.where(fast, math.log(1.0 / 32.0), math.log(0.1 / TOKENS)) + jitter[0]
    offset = jnp.where(fast, 0.0, math.log(0.3 * HEAD / TOKENS)) + jitter[1]
    return jnp.clip(jnp.stack([decay_rate, offset]), -20.0, 1.0).astype(jnp.float32)


def draw_log_decay_increments(key, part):
    count = TOKENS // TOK_DEV
    factors = jnp.exp(jax.random.uniform(jax.random.fold_in(key, 401), (count,), jnp.float32, math.log(0.1), math.log(0.8)))
    baseline_value = -jnp.repeat(factors, TOK_DEV, total_repeat_length=TOKENS) / TOKENS
    places = jax.random.randint(jax.random.fold_in(key, 402), (2,), 0, TOKENS)
    decay_losses = jnp.log(1.0 - jax.random.uniform(jax.random.fold_in(key, 403), (DELTA_HEADS, 2), jnp.float32, 0.2, 0.5))
    match_scores = (jnp.arange(TOKENS)[None, :] == places[:, None]).astype(jnp.float32)
    decay_increments = jnp.dot(decay_losses, match_scores, precision=lax.Precision.HIGHEST)
    return jnp.clip(baseline_value[None, :] + decay_increments, -2.0, 0.0).astype(jnp.float32)


def steps_of(rng, dims, pieces, smallest, top_value):
    level, own = 1.0, jax.random.fold_in(rng, 6)
    for axis_at, blocks in pieces:
        steps = jnp.exp(jax.random.uniform(jax.random.fold_in(own, axis_at), (blocks,), jnp.float32, smallest / len(pieces), top_value / len(pieces)))
        level = level * jnp.repeat(steps, dims[axis_at] // blocks).reshape([-1 if axis == axis_at else 1 for axis in range(len(dims))])
    return level


def scatter_about(own_key, extent, deviation, most, cuts=(), kind=jnp.bfloat16):
    values = jax.random.normal(own_key, extent, jnp.float32) * deviation
    if len(cuts) > 0:
        values = steps_of(own_key, extent, cuts, -0.22, 0.18) * values
    return jnp.clip(values, min=-most, max=most).astype(kind)


def setup_inputs(seed: int = 0) -> dict:
    arg_keys = jax.random.split(jax.random.key(seed), 17)
    return {
        "tokens": draw_tokens(jax.random.fold_in(arg_keys[16], 71), 0),
        "input_norm_gain": jnp.clip(1.0 + 0.18 * jax.random.normal(arg_keys[1], (D,), jnp.float32), 0.1, 1.9),
        "delta_query_weight": scatter_about(arg_keys[2], (D, DELTA_HEADS * HEAD), D ** -0.5, 0.125, ((0, 16), (1, 2))),
        "delta_key_weight": scatter_about(arg_keys[3], (D, DELTA_HEADS * HEAD), D ** -0.5, 0.125, ((0, 16), (1, 2))),
        "delta_value_weight": scatter_about(arg_keys[4], (D, DELTA_HEADS * HEAD), D ** -0.5, 0.125, ((0, 16), (1, 2))),
        "gate_weight": scatter_about(arg_keys[5], (D, 4, DELTA_HEADS), D ** -0.5, 0.125),
        "head_decay_params": draw_head_decay_params(jax.random.fold_in(arg_keys[16], 71), 0),
        "log_decay_increments": draw_log_decay_increments(jax.random.fold_in(arg_keys[16], 71), 0),
        "starting_state": scatter_about(arg_keys[8], (2, DELTA_HEADS, HEAD, HEAD), 0.1, 1.5, ((1, 2),), jnp.float32),
        "delta_norm_gain": jnp.clip(1.0 + 0.18 * jax.random.normal(arg_keys[9], (HEAD,), jnp.float32), 0.1, 1.9),
        "attention_query_weight": draw_attention_query_weight(jax.random.fold_in(arg_keys[16], 71), 0),
        "attention_key_weight": draw_attention_key_weight(jax.random.fold_in(arg_keys[16], 71), 0),
        "attention_value_weight": scatter_about(arg_keys[12], (D, KV_HEADS * HEAD), D ** -0.5, 0.125, ((0, 16), (1, 2))),
        "sink": jnp.clip(-1.0 + 4.0 * jax.random.uniform(arg_keys[13], (ATTN_HEADS,), jnp.float32) ** steps_of(arg_keys[13], (ATTN_HEADS,), ((0, 2),), -0.2, 0.2), -1.0, 3.0),
        "delta_output_weight": scatter_about(arg_keys[14], (DELTA_HEADS * HEAD, D), ((DELTA_HEADS + ATTN_HEADS) * HEAD) ** -0.5, 0.125, ((0, 2),)),
        "attention_output_weight": scatter_about(arg_keys[15], (ATTN_HEADS * HEAD, D), ((DELTA_HEADS + ATTN_HEADS) * HEAD) ** -0.5, 0.125, ((0, 2),)),
    }


EPS = 1e-06

def outer_product(spec, left, right):
    return jnp.einsum(spec, left, right, precision=lax.Precision.HIGHEST)

def unit_lower_inverse(lower):
    width = lower.shape[-1]
    inverse = jnp.eye(width, dtype=lower.dtype) - lower
    power = lower
    for turn in range(width.bit_length() - 2):
        power = outer_product('...ij,...jk->...ik', power, power)
        inverse = inverse + outer_product('...ij,...jk->...ik', inverse, power)
    return inverse

def block_terms(query_rows, keys, values, decay, strength):
    width = decay.shape[-1]
    summed_output = jnp.cumsum(decay, axis=-1)
    index = jnp.arange(width)
    inclusive = index[:, None] >= index[None, :]
    strict = index[:, None] > index[None, :]
    spread = summed_output[..., :, None] - summed_output[..., None, :]
    weights = jnp.where(inclusive, jnp.exp(jnp.where(inclusive, spread, 0.0)), 0.0)
    scaled_keys = keys * strength[..., None]
    lower = jnp.where(strict, outer_product('...ik,...jk->...ij', scaled_keys, keys) * weights, 0.0)
    inverse = unit_lower_inverse(lower)
    state_update = outer_product('...ij,...jv->...iv', inverse, values * strength[..., None])
    delta_correction = outer_product('...ij,...jk->...ik', inverse, scaled_keys * jnp.exp(summed_output)[..., None])
    mixing_output = outer_product('...ik,...jk->...ij', query_rows, keys) * weights
    return (summed_output, state_update, delta_correction, mixing_output)

def block_step(running_state, inputs):
    query_rows, keys, values, decay, strength = inputs
    summed_output, state_update, delta_correction, mixing_output = block_terms(query_rows, keys, values, decay, strength)
    fresh_values = state_update - outer_product('cpj,cjl->cpl', delta_correction, running_state)
    layer_output = outer_product('cpj,cjl->cpl', query_rows * jnp.exp(summed_output)[..., None], running_state) + outer_product('xgb,xbq->xgq', mixing_output, fresh_values)
    final_state = summed_output[:, -1]
    carried_state = keys * jnp.exp(final_state[:, None] - summed_output)[..., None]
    running_state = running_state * jnp.exp(final_state)[:, None, None] + outer_product('tmn,tml->tnl', carried_state, fresh_values)
    return (running_state, layer_output)

def delta_direction(query_rows, keys, values, decay, strength, start):
    heads, length, width = query_rows.shape
    count = length // BLOCK

    def split(array):
        return jnp.moveaxis(array.reshape((heads, count, BLOCK) + array.shape[2:]), 1, 0)
    final, outputs = lax.scan(block_step, start, (split(query_rows), split(keys), split(values), split(decay), split(strength)))
    return jnp.moveaxis(outputs, 0, 1).reshape(heads, length, width)

def reverse(array):
    return jnp.flip(array, axis=1)

def heads_first(array):
    rows = array.shape[0]
    return jnp.transpose(array.astype(jnp.float32).reshape(rows, -1, HEAD), (1, 0, 2))

def unit_rows(array):
    return array * lax.rsqrt(lax.optimization_barrier(jnp.sum(array * array, axis=-1, keepdims=True)) + EPS)

def reference(tokens, input_norm_gain, delta_query_weight, delta_key_weight, delta_value_weight, gate_weight, head_decay_params, log_decay_increments, starting_state, delta_norm_gain, attention_query_weight, attention_key_weight, attention_value_weight, sink, delta_output_weight, attention_output_weight):
    wide = tokens.astype(jnp.float32)
    normed = (wide * lax.rsqrt(lax.optimization_barrier(jnp.mean(wide * wide, axis=-1, keepdims=True)) + EPS) * input_norm_gain).astype(jnp.bfloat16)

    def project(weight):
        return jnp.dot(normed, weight, preferred_element_type=jnp.float32).astype(jnp.bfloat16)
    delta_query = project(delta_query_weight)
    delta_key = project(delta_key_weight)
    delta_value = project(delta_value_weight)
    attn_query = project(attention_query_weight)
    attn_key = project(attention_key_weight)
    attn_value = project(attention_value_weight)
    gate_values = jnp.dot(normed, gate_weight.reshape(D, 4 * DELTA_HEADS), preferred_element_type=jnp.float32).reshape(TOKENS, 4, DELTA_HEADS)
    query_rows = unit_rows(heads_first(delta_query)) * HEAD ** (-0.5)
    keys = unit_rows(heads_first(delta_key))
    values = heads_first(delta_value)
    decay_rates = jnp.exp(head_decay_params[0])[:, None]
    onward_decay_factor = -decay_rates * jax.nn.softplus(gate_values[:, 0, :].T) + log_decay_increments
    reverse_decay_factor = -decay_rates * jax.nn.softplus(gate_values[:, 1, :].T) + log_decay_increments
    forward_strength = jax.nn.sigmoid(gate_values[:, 2, :].T + head_decay_params[1][:, None])
    backward_strength = jax.nn.sigmoid(gate_values[:, 3, :].T + head_decay_params[1][:, None])
    forward_out = delta_direction(query_rows, keys, values, onward_decay_factor, forward_strength, starting_state[0])
    backward_out = reverse(delta_direction(reverse(query_rows), reverse(keys), reverse(values), reverse(reverse_decay_factor), reverse(backward_strength), starting_state[1]))
    both = forward_out + backward_out
    normal_out = both * lax.rsqrt(lax.optimization_barrier(jnp.mean(both * both, axis=-1, keepdims=True)) + EPS) * delta_norm_gain
    delta_out = jnp.transpose(normal_out, (1, 0, 2)).reshape(TOKENS, DELTA_HEADS * HEAD).astype(jnp.bfloat16)
    group = ATTN_HEADS // KV_HEADS
    keys_attn = attn_key.reshape(TOKENS, KV_HEADS, HEAD)
    values_attn = attn_value.reshape(TOKENS, KV_HEADS, HEAD)
    padded_keys = jnp.pad(keys_attn, ((WINDOW, WINDOW), (0, 0), (0, 0)))
    padded_values = jnp.pad(values_attn, ((WINDOW, WINDOW), (0, 0), (0, 0)))
    slopes = jnp.exp2(-8.0 * jnp.arange(1, ATTN_HEADS + 1, dtype=jnp.float32) / ATTN_HEADS).reshape(KV_HEADS, group, 1, 1)
    sink_logit = sink.reshape(KV_HEADS, group, 1, 1)
    reach = BLOCK + 2 * WINDOW

    def one_block(start):
        grouped = lax.dynamic_slice_in_dim(attn_query, start, BLOCK, 0).reshape(BLOCK, KV_HEADS, group, HEAD)
        near_keys = lax.dynamic_slice_in_dim(padded_keys, start, reach, 0)
        near_values = lax.dynamic_slice_in_dim(padded_values, start, reach, 0)
        scores = jnp.einsum('qhge,khe->hgqk', grouped.astype(jnp.float32), near_keys.astype(jnp.float32)) * HEAD ** (-0.5)
        target = start + jnp.arange(BLOCK, dtype=jnp.int32)
        source = start - WINDOW + jnp.arange(reach, dtype=jnp.int32)
        distance = jnp.abs(target[:, None] - source[None, :])
        valid = (distance <= WINDOW) & (source[None, :] >= 0) & (source[None, :] < TOKENS)
        scores = jnp.where(valid, scores - slopes * distance.astype(jnp.float32), -jnp.inf)
        top = jnp.maximum(lax.optimization_barrier(jnp.max(scores, axis=-1, keepdims=True)), sink_logit)
        weights = jnp.exp(scores - top)
        probs = (weights / (lax.optimization_barrier(jnp.sum(weights, axis=-1, keepdims=True)) + jnp.exp(sink_logit - top))).astype(jnp.bfloat16)
        result = jnp.einsum('hgqk,khe->qhge', probs.astype(jnp.float32), near_values.astype(jnp.float32))
        return result.astype(jnp.bfloat16).reshape(BLOCK, ATTN_HEADS * HEAD)
    starts = jnp.arange(TOKENS // BLOCK, dtype=jnp.int32) * BLOCK
    attn_out = lax.map(one_block, starts).reshape(TOKENS, ATTN_HEADS * HEAD)
    delta_rows = DELTA_HEADS * HEAD // N_TP
    attn_rows = ATTN_HEADS * HEAD // N_TP
    total = jnp.zeros((TOKENS, D), jnp.float32)
    for index in range(N_TP):
        part_sum = jnp.dot(delta_out[:, index * delta_rows:(index + 1) * delta_rows], delta_output_weight[index * delta_rows:(index + 1) * delta_rows], preferred_element_type=jnp.float32)
        part_sum = part_sum + jnp.dot(attn_out[:, index * attn_rows:(index + 1) * attn_rows], attention_output_weight[index * attn_rows:(index + 1) * attn_rows], preferred_element_type=jnp.float32)
        total = total + lax.optimization_barrier(part_sum.astype(jnp.bfloat16)).astype(jnp.float32)
    return total.astype(jnp.bfloat16)
```

```python
import functools

import jax
import jax.numpy as jnp
from jax import lax
from jax.experimental import pallas as pl
from jax.experimental.pallas import tpu as pltpu
from jax.sharding import PartitionSpec as P

HEAD = 64
WINDOW = 128
EPS = 1e-06
F32 = jnp.float32
BF16 = jnp.bfloat16


def ring_dims(mesh):
    names = list(mesh.axis_names)
    count = mesh.shape["sp"]
    devices = mesh.devices
    at = names.index("sp")
    line = [devices[tuple(i if k == at else 0 for k in range(len(names)))] for i in range(count)]
    try:
        coords = [tuple(d.coords) for d in line]
        dims = []
        for axis in range(len(coords[0])):
            size = len({c[axis] for c in coords})
            if size > 1:
                first = coords[0][axis]
                stride = next(i for i in range(count) if coords[i][axis] != first)
                dims.append((size, stride))
        dims.sort(key=lambda d: -d[1])
        total = 1
        for size, stride in reversed(dims):
            if stride != total:
                return ((count, 1),)
            total *= size
        return tuple(dims) if total == count else ((count, 1),)
    except Exception:
        return ((count, 1),)


def tree(dims, order, lean):
    zero = (0,) * len(dims)
    nodes, level = [], [zero]
    held = [zero]
    for d in order:
        size = dims[d][0]
        up = size // 2 if lean else (size - 1) // 2
        down = size - 1 - up
        for far in range(1, max(up, down) + 1):
            for base in held:
                for step, reach in ((1, up), (-1, down)):
                    if far <= reach:
                        here, parent = list(base), list(base)
                        here[d] = (step * far) % size
                        parent[d] = (step * (far - 1)) % size
                        nodes.append((tuple(here), tuple(parent), d, step))
        held = [b[:d] + (r,) + b[d + 1 :] for b in held for r in range(size)]
    return nodes


def piece_trees(dims, pieces):
    count = len(dims)
    fore = list(range(count))
    orders = [fore, fore[:1] + fore[1:][::-1], fore[1:] + fore[:1], fore[1:][::-1] + fore[:1]]
    return [tree(dims, orders[p % 4], p % 2 == 0) for p in range(pieces)]


def dot(left, right, dims=((1,), (0,))):
    return lax.dot_general(
        left.astype(BF16), right.astype(BF16), (dims, ((), ())), preferred_element_type=F32
    )


def exact_dot(left, right, dims):
    return lax.dot_general(
        left, right, (dims, ((), ())), precision=lax.Precision.HIGHEST, preferred_element_type=F32
    )


def kernel(
    cfg,
    tokens_ref,
    gain_ref,
    gate_ref,
    params_ref,
    increments_ref,
    start_ref,
    norm_gain_ref,
    logits_ref,
    wd_ref,
    wa_ref,
    delta_out_hbm,
    attn_out_hbm,
    out_ref,
    norm3,
    dbuf,
    abuf,
    dacc,
    aacc,
    proj,
    aq,
    kv,
    halo,
    mine,
    maps,
    state,
    base_out,
    reads,
    feats,
    wo,
    partial,
    prec,
    d_send,
    d_recv,
    a_send,
    a_recv,
    m_send,
    m_recv,
    h_send,
    h_recv,
    p_send,
    p_recv,
    w_sem,
):
    n, ntp, dims, heads, attn_heads, key_heads = cfg
    me, mt = lax.axis_index("sp"), lax.axis_index("tp")
    rows, width = tokens_ref.shape
    kd = width // n
    dcols, acols = heads * HEAD, attn_heads * HEAD
    kcols = key_heads * HEAD

    barrier = pltpu.get_barrier_semaphore()
    for k in range(1, n):
        pl.semaphore_signal(barrier, inc=1, device_id={"sp": lax.rem(me + k, n)})
    for k in range(1, ntp):
        pl.semaphore_signal(barrier, inc=1, device_id={"tp": lax.rem(mt + k, ntp)})
    pl.semaphore_wait(barrier, n - 1 + ntp - 1)

    def shifted(d, step):
        size, stride = dims[d]
        digit = lax.rem(me // stride, size)
        return me + (lax.rem(digit + step + size, size) - digit) * stride

    def slot(offset):
        at = 0
        for (size, stride), o in zip(dims, offset):
            at = at + o * stride
        return at

    def source(offset):
        at = 0
        for (size, stride), o in zip(dims, offset):
            digit = lax.rem(me // stride, size)
            at = at + lax.rem(digit - o + size, size) * stride
        return at

    def gather(own, buf, send, recv):
        trees = piece_trees(dims, buf.shape[0])
        started = []

        def copy(p, node):
            here, parent, d, step = node
            a, b = slot(parent), slot(here)
            return pltpu.make_async_remote_copy(
                src_ref=own.at[p] if a == 0 else buf.at[p, a],
                dst_ref=buf.at[p, b],
                send_sem=send.at[p, b],
                recv_sem=recv.at[p, b],
                device_id={"sp": shifted(d, step)},
            )

        def forward(p, offset):
            for node in trees[p]:
                if node[1] == offset:
                    made = copy(p, node)
                    made.start()
                    started.append(made)

        def begin():
            for p in range(len(trees)):
                forward(p, (0,) * len(dims))

        def arrive(index, acc):
            for p in range(len(trees)):
                copy(p, trees[p][index]).wait_recv()
                forward(p, trees[p][index][0])
            for p in range(len(trees)):
                here = trees[p][index][0]
                acc[p] += dot(norm3[source(here)], buf[p, slot(here)])

        return begin, arrive, started

    d_begin, d_arrive, d_started = gather(wd_ref, dbuf, d_send, d_recv)
    a_begin, a_arrive, a_started = gather(wa_ref, abuf, a_send, a_recv)
    d_begin()
    w_copies = [
        pltpu.make_async_copy(delta_out_hbm, wo.at[0], w_sem.at[0]),
        pltpu.make_async_copy(attn_out_hbm, wo.at[1], w_sem.at[1]),
    ]
    for made in w_copies:
        made.start()

    wide = tokens_ref[...].astype(F32)
    normed = (
        wide * lax.rsqrt(jnp.mean(wide * wide, axis=-1, keepdims=True) + EPS) * gain_ref[...]
    ).astype(BF16)
    for j in range(n):
        norm3[j] = normed[:, j * kd : (j + 1) * kd]
    gates = dot(gate_ref[...], normed, ((1,), (1,)))
    rates = jnp.exp(params_ref[:, 0:1])
    offsets = params_ref[:, 1:2]
    row = lax.broadcasted_iota(jnp.int32, (rows, rows), 0)
    col = lax.broadcasted_iota(jnp.int32, (rows, rows), 1)
    eye = (row == col).astype(F32)
    sums_row, sums_col, strength_col = [], [], []
    for r in range(2):
        x = gates[r * heads : (r + 1) * heads]
        soft = jnp.maximum(x, 0.0) + jnp.log1p(jnp.exp(-jnp.abs(x)))
        decay = increments_ref[...] - rates * soft
        y = gates[(2 + r) * heads : (3 + r) * heads] + offsets
        strength = 1.0 / (1.0 + jnp.exp(-y))
        tri = ((row >= col) if r == 0 else (row <= col)).astype(F32)
        sums_row.append(exact_dot(decay, tri, ((1,), (1,))))
        sums_col.append(exact_dot(tri, decay, ((1,), (1,))))
        strength_col.append(exact_dot(eye, strength, ((1,), (1,))))
    for p in range(wd_ref.shape[0]):
        dacc[p] = dot(norm3[me], wd_ref[p])
    for p in range(wa_ref.shape[0]):
        aacc[p] = dot(norm3[me], wa_ref[p])
    for index in range(n - 1):
        d_arrive(index, dacc)
    a_begin()
    per = dacc.shape[2]
    for p in range(dacc.shape[0]):
        proj[:, p * per : (p + 1) * per] = dacc[p].astype(BF16)

    lane = lax.broadcasted_iota(jnp.int32, (HEAD, 2 * HEAD), 1)
    sub = lax.broadcasted_iota(jnp.int32, (HEAD, 2 * HEAD), 0)
    turn = jnp.where(lane < HEAD, 1.0, -1.0)
    shift_eye = (lane == sub + HEAD).astype(F32)
    same = {s: (row // s) == (col // s) for s in (16, 32, 64, 128)}

    def delta_group(some):
        chains = []
        for h in some:
            q = proj[:, h * HEAD : (h + 1) * HEAD].astype(F32)
            k = proj[:, dcols + h * HEAD : dcols + (h + 1) * HEAD].astype(F32)
            v = proj[:, 2 * dcols + h * HEAD : 2 * dcols + (h + 1) * HEAD].astype(F32)
            q = q * (lax.rsqrt(jnp.sum(q * q, axis=-1, keepdims=True) + EPS) * HEAD ** (-0.5))
            k = k * lax.rsqrt(jnp.sum(k * k, axis=-1, keepdims=True) + EPS)
            gram = dot(k, k, ((1,), (1,)))
            cross = dot(q, k, ((1,), (1,)))
            for r in range(2):
                incl = (row >= col) if r == 0 else (row <= col)
                c_row = sums_row[r][h : h + 1, :]
                c_col = sums_col[r][:, h : h + 1]
                b_col = strength_col[r][:, h : h + 1]
                total = c_col[rows - 1 : rows] if r == 0 else c_col[0:1]
                w = jnp.exp(jnp.where(incl, c_col - c_row, -1e30))
                low = jnp.where(row == col, 0.0, gram * w) * b_col
                grown = jnp.exp(c_col)
                rhs = jnp.concatenate([v * b_col, k * (b_col * grown)], axis=1)
                chains.append(
                    dict(
                        h=h,
                        r=r,
                        low=low,
                        rhs=rhs,
                        mix=cross * w,
                        carried=k * jnp.exp(total - c_col),
                        q=q * grown,
                        total=total,
                    )
                )
        for c in chains:
            base = jnp.where(same[16], c["low"], 0.0)
            c["inv"], c["pow"] = eye - base, base
        for _ in range(3):
            for c in chains:
                c["pow"] = dot(c["pow"], c["pow"])
            for c in chains:
                c["inv"] = c["inv"] + dot(c["inv"], c["pow"])
        for s in (32, 64, 128):
            for c in chains:
                off = jnp.where(same[s] & jnp.logical_not(same[s // 2]), c["low"], 0.0)
                c["tmp"] = dot(off, c["inv"])
            for c in chains:
                c["inv"] = c["inv"] - dot(c["inv"], c["tmp"])
        for c in chains:
            c["uw"] = dot(c["inv"], c["rhs"])
        for c in chains:
            mapped = dot(c["carried"], c["uw"], ((0,), (0,))) * turn
            mapped = mapped + shift_eye * jnp.exp(c["total"])
            mine[c["r"], c["h"]] = mapped.astype(BF16)
            c["read"] = dot(c["mix"], c["uw"])
        for f, b in zip(chains[::2], chains[1::2]):
            base_out[f["h"]] = f["read"][:, :HEAD] + b["read"][:, :HEAD]
            reads[f["h"]] = jnp.concatenate(
                [f["q"] - f["read"][:, HEAD:], b["q"] - b["read"][:, HEAD:]], axis=1
            ).astype(BF16)

    batch = min(2, heads)
    groups = heads // batch
    done = 0
    for g in range(groups):
        delta_group(range(g * batch, (g + 1) * batch))
        upto = (n - 1) * (g + 1) // groups if g < groups - 1 else done
        while done < upto:
            a_arrive(done, aacc)
            done += 1

    m_copies = []
    for k in range(1, n):
        made = pltpu.make_async_remote_copy(
            src_ref=mine.at[(me + k) // n],
            dst_ref=maps.at[me],
            send_sem=m_send.at[k],
            recv_sem=m_recv.at[me],
            device_id={"sp": lax.rem(me + k, n)},
        )
        made.start()
        m_copies.append(made)

    while done < n - 1:
        a_arrive(done, aacc)
        done += 1
    per_a = aacc.shape[2]
    for p in range(aacc.shape[0]):
        prec[:, p * per_a : (p + 1) * per_a] = aacc[p].astype(BF16)
    kv[...] = prec[:, acols : acols + 2 * kcols]
    h_copies = []
    for at, step in ((0, 1), (1, n - 1)):
        made = pltpu.make_async_remote_copy(
            src_ref=kv,
            dst_ref=halo.at[at],
            send_sem=h_send.at[at],
            recv_sem=h_recv.at[at],
            device_id={"sp": lax.rem(me + step, n)},
        )
        made.start()
        h_copies.append(made)
    for made in h_copies:
        made.wait_recv()

    gap = (row - col).astype(F32)
    far_low, far_high = gap + rows, rows - gap
    ok_low = (far_low <= WINDOW) & (me > 0)
    ok_high = (far_high <= WINDOW) & (me < n - 1)
    bias = [
        jnp.where(ok_low, far_low, 1e30),
        jnp.where(jnp.abs(gap) <= WINDOW, jnp.abs(gap), 1e30),
        jnp.where(ok_high, far_high, 1e30),
    ]
    share = attn_heads // key_heads
    for h in range(attn_heads):
        at = (h // share) * HEAD
        q = prec[:, h * HEAD : (h + 1) * HEAD]
        slope = logits_ref[h : h + 1, 0:1]
        sink = logits_ref[h : h + 1, 1:2]
        parts = [halo.at[0], kv, halo.at[1]]
        keys = [part[:, at : at + HEAD] for part in parts]
        vals = [part[:, kcols + at : kcols + at + HEAD] for part in parts]
        scores = [
            dot(q, k, ((1,), (1,))) * HEAD ** (-0.5) - slope * b for k, b in zip(keys, bias)
        ]
        top = jnp.maximum(jnp.maximum(scores[0], scores[1]), scores[2])
        top = jnp.maximum(jnp.max(top, axis=-1, keepdims=True), sink)
        weights = [jnp.exp(s - top) for s in scores]
        total = jnp.sum(weights[0] + weights[1] + weights[2], axis=-1, keepdims=True)
        scale = 1.0 / (total + jnp.exp(sink - top))
        res = dot(weights[0], vals[0]) + dot(weights[1], vals[1]) + dot(weights[2], vals[2])
        feats[:, dcols + h * HEAD : dcols + (h + 1) * HEAD] = (res * scale).astype(BF16)

    state[...] = start_ref[...]

    def apply(r, s):
        pltpu.make_async_remote_copy(
            src_ref=mine.at[0],
            dst_ref=maps.at[s],
            send_sem=m_send.at[0],
            recv_sem=m_recv.at[s],
            device_id={"sp": lax.rem(me + 1, n)},
        ).wait_recv()
        for h in range(heads):
            m = maps[s, h]
            now = state[r, h]
            high = now.astype(BF16)
            rest = (now - high.astype(F32)).astype(BF16)
            moved = dot(m[:, HEAD:], jnp.concatenate([high, rest], axis=1))
            state[r, h] = moved[:, :HEAD] + moved[:, HEAD:] + m[:, :HEAD].astype(F32)

    def forward_step(i, carry):
        apply(0, i)
        return carry

    def backward_step(i, carry):
        apply(1, n - 1 - i)
        return carry

    lax.fori_loop(0, me, forward_step, 0)
    lax.fori_loop(0, n - 1 - me, backward_step, 0)

    for h in range(heads):
        both = jnp.concatenate([state[0, h], state[1, h]], axis=0)
        y = base_out[h] + dot(reads[h], both)
        y = y * lax.rsqrt(jnp.mean(y * y, axis=-1, keepdims=True) + EPS) * norm_gain_ref[...]
        feats[:, h * HEAD : (h + 1) * HEAD] = y.astype(BF16)

    for made in w_copies:
        made.wait()
    step = min(512, width)
    each = rows // ntp
    for at in range(0, width, step):
        res = dot(feats[:, :dcols], wo[0, :, at : at + step]) + dot(
            feats[:, dcols:], wo[1, :, at : at + step]
        )
        res = res.astype(BF16)
        for p in range(ntp):
            partial[0, p, :, at : at + step] = res[p * each : (p + 1) * each]
    p_copies = []
    for k in range(1, ntp):
        peer = lax.rem(mt + k, ntp)
        made = pltpu.make_async_remote_copy(
            src_ref=partial.at[0, peer],
            dst_ref=partial.at[1, k],
            send_sem=p_send.at[k],
            recv_sem=p_recv.at[k],
            device_id={"tp": peer},
        )
        made.start()
        p_copies.append(made)
    total = partial[0, mt].astype(F32)
    for k in range(1, ntp):
        p_copies[k - 1].wait_recv()
        total = total + partial[1, k].astype(F32)
    out_ref[...] = total.astype(BF16)
    for made in d_started + a_started + m_copies + h_copies + p_copies:
        made.wait_send()


def cut(weights):
    joined = jnp.concatenate(weights, axis=1)
    rows, cols = joined.shape
    pieces = 4 if cols % 512 == 0 else 1
    return jnp.transpose(joined.reshape(rows, pieces, cols // pieces), (1, 0, 2))


def on_device(
    dims,
    tokens,
    input_norm_gain,
    delta_query_weight,
    delta_key_weight,
    delta_value_weight,
    gate_weight,
    head_decay_params,
    log_decay_increments,
    starting_state,
    delta_norm_gain,
    attention_query_weight,
    attention_key_weight,
    attention_value_weight,
    sink,
    delta_output_weight,
    attention_output_weight,
):
    n, ntp = lax.axis_size("sp"), lax.axis_size("tp")
    rows, width = tokens.shape
    heads = delta_query_weight.shape[1] // HEAD
    attn_heads = attention_query_weight.shape[1] // HEAD
    key_heads = attention_key_weight.shape[1] // HEAD
    gates = lax.dynamic_slice_in_dim(gate_weight, lax.axis_index("tp") * heads, heads, 2)
    gates = gates.reshape(gate_weight.shape[0], 4 * heads).T
    wd = cut([delta_query_weight, delta_key_weight, delta_value_weight])
    wa = cut([attention_query_weight, attention_key_weight, attention_value_weight])
    head_ids = (lax.axis_index("tp") * attn_heads + jnp.arange(attn_heads)).astype(F32)
    slopes = jnp.exp2(-8.0 * (head_ids + 1.0) / (attn_heads * ntp))
    logits = jnp.stack([slopes, sink], axis=1)
    cfg = (n, ntp, dims, heads, attn_heads, key_heads)
    dcols, acols, kcols = heads * HEAD, attn_heads * HEAD, key_heads * HEAD
    pd, pa = wd.shape[0], wa.shape[0]
    vmem = pl.BlockSpec(memory_space=pltpu.VMEM)
    hbm = pl.BlockSpec(memory_space=pl.ANY)
    dma = pltpu.SemaphoreType.DMA
    return pl.pallas_call(
        functools.partial(kernel, cfg),
        out_shape=jax.ShapeDtypeStruct((rows // ntp, width), BF16),
        in_specs=[vmem] * 10 + [hbm] * 2,
        out_specs=vmem,
        scratch_shapes=[
            pltpu.VMEM((n, rows, width // n), BF16),
            pltpu.VMEM((pd, n) + wd.shape[1:], BF16),
            pltpu.VMEM((pa, n) + wa.shape[1:], BF16),
            pltpu.VMEM((pd, rows, wd.shape[2]), F32),
            pltpu.VMEM((pa, rows, wa.shape[2]), F32),
            pltpu.VMEM((rows, 3 * dcols), BF16),
            pltpu.VMEM((8, 128), BF16),
            pltpu.VMEM((rows, 2 * kcols), BF16),
            pltpu.VMEM((2, rows, 2 * kcols), BF16),
            pltpu.VMEM((2, heads, HEAD, 2 * HEAD), BF16),
            pltpu.VMEM((n, heads, HEAD, 2 * HEAD), BF16),
            pltpu.VMEM((2, heads, HEAD, HEAD), F32),
            pltpu.VMEM((heads, rows, HEAD), F32),
            pltpu.VMEM((heads, rows, 2 * HEAD), BF16),
            pltpu.VMEM((rows, dcols + acols), BF16),
            pltpu.VMEM((2,) + delta_output_weight.shape, BF16),
            pltpu.VMEM((2, ntp, rows // ntp, width), BF16),
            pltpu.VMEM((rows, acols + 2 * kcols), BF16),
            dma((pd, n)),
            dma((pd, n)),
            dma((pa, n)),
            dma((pa, n)),
            dma((n,)),
            dma((n,)),
            dma((2,)),
            dma((2,)),
            dma((ntp,)),
            dma((ntp,)),
            dma((2,)),
        ],
        compiler_params=pltpu.CompilerParams(
            collective_id=0, has_side_effects=True, vmem_limit_bytes=60 * 1024 * 1024
        ),
    )(
        tokens,
        input_norm_gain.reshape(1, -1),
        gates,
        head_decay_params.T,
        log_decay_increments,
        starting_state,
        delta_norm_gain.reshape(1, -1),
        logits,
        wd,
        wa,
        delta_output_weight,
        attention_output_weight,
    )


def solution(mesh):
    in_specs = (
        P("sp", None),
        P(),
        P("sp", "tp"),
        P("sp", "tp"),
        P("sp", "tp"),
        P(),
        P(None, "tp"),
        P("tp", "sp"),
        P(None, "tp", None, None),
        P(),
        P("sp", "tp"),
        P("sp", "tp"),
        P("sp", "tp"),
        P("tp"),
        P("tp", None),
        P("tp", None),
    )
    out_specs = P(("sp", "tp"), None)
    return jax.shard_map(
        functools.partial(on_device, ring_dims(mesh)),
        mesh=mesh,
        in_specs=in_specs,
        out_specs=out_specs,
        check_vma=False,
    )
```

```python
import functools

import jax
import jax.numpy as jnp
from jax import lax
from jax.experimental import pallas as pl
from jax.experimental.pallas import tpu as pltpu
from jax.sharding import PartitionSpec as P

HEAD = 64
WINDOW = 128
EPS = 1e-06
F32 = jnp.float32
BF16 = jnp.bfloat16


def ring_dims(mesh):
    names = list(mesh.axis_names)
    count = mesh.shape["sp"]
    devices = mesh.devices
    at = names.index("sp")
    line = [devices[tuple(i if k == at else 0 for k in range(len(names)))] for i in range(count)]
    try:
        coords = [tuple(d.coords) for d in line]
        dims = []
        for axis in range(len(coords[0])):
            size = len({c[axis] for c in coords})
            if size > 1:
                first = coords[0][axis]
                stride = next(i for i in range(count) if coords[i][axis] != first)
                dims.append((size, stride))
        dims.sort(key=lambda d: -d[1])
        total = 1
        for size, stride in reversed(dims):
            if stride != total:
                return ((count, 1),)
            total *= size
        return tuple(dims) if total == count else ((count, 1),)
    except Exception:
        return ((count, 1),)


def piece_orders(dims, pieces):
    count = len(dims)
    if count == 3:
        orders = [(2, 0, 1), (1, 0, 2)]
    elif count == 2:
        orders = [(0, 1), (1, 0)]
    else:
        orders = [tuple(range(count))]
    return [orders[p % len(orders)] for p in range(pieces)]


def arrivals(dims, order):
    held, nodes = [(0,) * len(dims)], []
    for d in order:
        size = dims[d][0]
        turns = sorted(range(1, size), key=lambda r: (min(r, size - r), r))
        nodes += [(b[:d] + (r,) + b[d + 1 :], d) for r in turns for b in held]
        held = [b[:d] + (r,) + b[d + 1 :] for b in held for r in range(size)]
    return nodes


def dot(left, right, dims=((1,), (0,))):
    return lax.dot_general(
        left.astype(BF16), right.astype(BF16), (dims, ((), ())), preferred_element_type=F32
    )


def exact_dot(left, right, dims):
    return lax.dot_general(
        left, right, (dims, ((), ())), precision=lax.Precision.HIGHEST, preferred_element_type=F32
    )


def kernel(
    cfg,
    tokens_ref,
    gain_ref,
    gate_ref,
    params_ref,
    increments_ref,
    start_ref,
    norm_gain_ref,
    logits_ref,
    *refs,
):
    parts = cfg[-2:]
    count = parts[0] + parts[1]
    w_refs, refs = refs[:count], refs[count:]
    (
        delta_out_hbm,
        attn_out_hbm,
        out_ref,
        norm3,
        dbuf,
        abuf,
        dacc,
        aacc,
        proj,
        aq,
        kv,
        halo,
        mine,
        maps,
        state,
        base_out,
        reads,
        feats,
        wo,
        partial,
        prec,
        d_send,
        d_recv,
        a_send,
        a_recv,
        m_send,
        m_recv,
        h_send,
        h_recv,
        p_send,
        p_recv,
        w_sem,
    ) = refs
    n, ntp, dims, heads, attn_heads, key_heads = cfg[:6]
    me, mt = lax.axis_index("sp"), lax.axis_index("tp")
    rows, width = tokens_ref.shape
    kd = width // n
    half = mine.shape[2]
    dcols, acols = heads * HEAD, attn_heads * HEAD
    kcols = key_heads * HEAD

    barrier = pltpu.get_barrier_semaphore()
    for k in range(1, n):
        pl.semaphore_signal(barrier, inc=1, device_id={"sp": lax.rem(me + k, n)})
    for k in range(1, ntp):
        pl.semaphore_signal(barrier, inc=1, device_id={"tp": lax.rem(mt + k, ntp)})
    pl.semaphore_wait(barrier, n - 1 + ntp - 1)

    def shifted(d, step):
        size, stride = dims[d]
        digit = lax.rem(me // stride, size)
        return me + (lax.rem(digit + step + size, size) - digit) * stride

    def slot(offset):
        at = 0
        for (size, stride), o in zip(dims, offset):
            at = at + o * stride
        return at

    def source(offset):
        at = 0
        for (size, stride), o in zip(dims, offset):
            digit = lax.rem(me // stride, size)
            at = at + lax.rem(digit - o + size, size) * stride
        return at

    def digit(d):
        return lax.rem(me // dims[d][1], dims[d][0])

    def gather(own, buf, send, recv, typed=False):
        orders = piece_orders(dims, buf.shape[0])
        lists = [arrivals(dims, order) for order in orders]
        started = []

        def copy(p, parent, here, d, step):
            a, b = slot(parent), slot(here)
            src = own[p] if a == 0 else buf.at[p, a]
            dst = buf.at[p, b]
            if typed and here[0] != 0:
                size = dims[0][0]
                if d == 0 and size > 2:
                    kind = 0 if step > 0 else 1
                elif d == 0:
                    kind = digit(0)
                else:
                    kind = (size - 1 + here[0] - digit(0)) // size
                src, dst = src.at[kind], dst.at[kind]
            return pltpu.make_async_remote_copy(
                src_ref=src,
                dst_ref=dst,
                send_sem=send.at[p, b + (0 if step > 0 else n)],
                recv_sem=recv.at[p, b],
                device_id={"sp": me + step * dims[d][1] if dims[d][0] > 2 else shifted(d, 1)},
            )

        def launch(p, parent, d):
            size, now = dims[d][0], parent[d]
            if size == 2:
                if now == 0:
                    moves = [(1, None)]
                else:
                    moves = []
            else:
                at = digit(d)
                moves = []
                if now + 1 < size:
                    moves.append((1, (at < size - 1) & (at >= now)))
                if now == 0:
                    moves.append((-1, at > 0))
                elif now > 1:
                    moves.append((-1, (at > 0) & (at < now)))
            for step, when in moves:
                here = parent[:d] + ((now + step) % size,) + parent[d + 1 :]
                made = copy(p, parent, here, d, step)
                if when is None:
                    made.start()
                else:
                    pl.when(when)(made.start)
                started.append((made, when))

        def begin():
            for p, order in enumerate(orders):
                for d in order:
                    launch(p, (0,) * len(dims), d)

        def arrive(index, use):
            for p, order in enumerate(orders):
                here, d = lists[p][index]
                copy(p, here, here, d, 1).wait_recv()
                for later in order[order.index(d) :]:
                    launch(p, here, later)
            if use is not None:
                for p in range(len(orders)):
                    here = lists[p][index][0]
                    use[p] += dot(norm3[source(here)], buf[p, slot(here)])

        def finish():
            for made, when in started:
                if when is None:
                    made.wait_send()
                else:
                    pl.when(when)(made.wait_send)

        return begin, arrive, finish

    def views(weights, pieces, each):
        if len(weights) == 1:
            return [weights[0].at[p] for p in range(pieces)]
        return [w.at[:, c : c + each] for w in weights for c in range(0, w.shape[1], each)]

    wd_own = views(w_refs[: parts[0]], dbuf.shape[0], dbuf.shape[3])
    wa_own = views(w_refs[parts[0] :], abuf.shape[0], abuf.shape[3])
    m_own = [mine.at[p] for p in range(mine.shape[0])]
    d_begin, d_arrive, d_finish = gather(wd_own, dbuf, d_send, d_recv)
    a_begin, a_arrive, a_finish = gather(wa_own, abuf, a_send, a_recv)
    m_begin, m_arrive, m_finish = gather(m_own, maps, m_send, m_recv, typed=True)
    d_begin()
    w_copies = [
        pltpu.make_async_copy(delta_out_hbm, wo.at[0], w_sem.at[0]),
        pltpu.make_async_copy(attn_out_hbm, wo.at[1], w_sem.at[1]),
    ]
    for made in w_copies:
        made.start()

    wide = tokens_ref[...].astype(F32)
    normed = (
        wide * lax.rsqrt(jnp.mean(wide * wide, axis=-1, keepdims=True) + EPS) * gain_ref[...]
    ).astype(BF16)
    for j in range(n):
        norm3[j] = normed[:, j * kd : (j + 1) * kd]
    gates = dot(gate_ref[...], normed, ((1,), (1,)))
    rates = jnp.exp(params_ref[:, 0:1])
    offsets = params_ref[:, 1:2]
    row = lax.broadcasted_iota(jnp.int32, (rows, rows), 0)
    col = lax.broadcasted_iota(jnp.int32, (rows, rows), 1)
    eye = (row == col).astype(F32)
    sums_row, sums_col, strength_col = [], [], []
    for r in range(2):
        x = gates[r * heads : (r + 1) * heads]
        soft = jnp.maximum(x, 0.0) + jnp.log1p(jnp.exp(-jnp.abs(x)))
        decay = increments_ref[...] - rates * soft
        y = gates[(2 + r) * heads : (3 + r) * heads] + offsets
        strength = 1.0 / (1.0 + jnp.exp(-y))
        tri = ((row >= col) if r == 0 else (row <= col)).astype(F32)
        sums_row.append(exact_dot(decay, tri, ((1,), (1,))))
        sums_col.append(exact_dot(tri, decay, ((1,), (1,))))
        strength_col.append(exact_dot(eye, strength, ((1,), (1,))))
    for p in range(dbuf.shape[0]):
        dacc[p] = dot(norm3[me], wd_own[p][...])
    for p in range(abuf.shape[0]):
        aacc[p] = dot(norm3[me], wa_own[p][...])
    for index in range(n - 1):
        d_arrive(index, dacc)
    a_begin()
    per = dacc.shape[2]
    for p in range(dacc.shape[0]):
        proj[:, p * per : (p + 1) * per] = dacc[p].astype(BF16)

    lane = lax.broadcasted_iota(jnp.int32, (HEAD, 2 * HEAD), 1)
    sub = lax.broadcasted_iota(jnp.int32, (HEAD, 2 * HEAD), 0)
    turn = jnp.where(lane < HEAD, 1.0, -1.0)
    shift_eye = (lane == sub + HEAD).astype(F32)
    same = {s: (row // s) == (col // s) for s in (16, 32, 64, 128)}

    def delta_group(some):
        chains = []
        for h in some:
            q = proj[:, h * HEAD : (h + 1) * HEAD].astype(F32)
            k = proj[:, dcols + h * HEAD : dcols + (h + 1) * HEAD].astype(F32)
            v = proj[:, 2 * dcols + h * HEAD : 2 * dcols + (h + 1) * HEAD].astype(F32)
            q = q * (lax.rsqrt(jnp.sum(q * q, axis=-1, keepdims=True) + EPS) * HEAD ** (-0.5))
            k = k * lax.rsqrt(jnp.sum(k * k, axis=-1, keepdims=True) + EPS)
            gram = dot(k, k, ((1,), (1,)))
            cross = dot(q, k, ((1,), (1,)))
            for r in range(2):
                incl = (row >= col) if r == 0 else (row <= col)
                c_row = sums_row[r][h : h + 1, :]
                c_col = sums_col[r][:, h : h + 1]
                b_col = strength_col[r][:, h : h + 1]
                total = c_col[rows - 1 : rows] if r == 0 else c_col[0:1]
                w = jnp.exp(jnp.where(incl, c_col - c_row, -1e30))
                low = jnp.where(row == col, 0.0, gram * w) * b_col
                grown = jnp.exp(c_col)
                rhs = jnp.concatenate([v * b_col, k * (b_col * grown)], axis=1)
                chains.append(
                    dict(
                        h=h,
                        r=r,
                        low=low,
                        rhs=rhs,
                        mix=cross * w,
                        carried=k * jnp.exp(total - c_col),
                        q=q * grown,
                        total=total,
                    )
                )
        for c in chains:
            base = jnp.where(same[16], c["low"], 0.0)
            c["inv"], c["pow"] = eye - base, base
        for _ in range(3):
            for c in chains:
                c["pow"] = dot(c["pow"], c["pow"])
            for c in chains:
                c["inv"] = c["inv"] + dot(c["inv"], c["pow"])
        for s in (32, 64, 128):
            for c in chains:
                off = jnp.where(same[s] & jnp.logical_not(same[s // 2]), c["low"], 0.0)
                c["tmp"] = dot(off, c["inv"])
            for c in chains:
                c["inv"] = c["inv"] - dot(c["inv"], c["tmp"])
        for c in chains:
            c["uw"] = dot(c["inv"], c["rhs"])
        for c in chains:
            mapped = dot(c["carried"], c["uw"], ((0,), (0,))) * turn
            mapped = mapped + shift_eye * jnp.exp(c["total"])
            mine[c["h"] // half, c["r"], c["h"] % half] = mapped.astype(BF16)
            c["read"] = dot(c["mix"], c["uw"])
        for f, b in zip(chains[::2], chains[1::2]):
            base_out[f["h"]] = f["read"][:, :HEAD] + b["read"][:, :HEAD]
            reads[f["h"]] = jnp.concatenate(
                [f["q"] - f["read"][:, HEAD:], b["q"] - b["read"][:, HEAD:]], axis=1
            ).astype(BF16)

    batch = min(2, heads)
    groups = heads // batch
    done = 0
    for g in range(groups):
        delta_group(range(g * batch, (g + 1) * batch))
        upto = (n - 1) * (g + 1) // groups if g < groups - 1 else done
        while done < upto:
            a_arrive(done, aacc)
            done += 1

    m_begin()
    while done < n - 1:
        a_arrive(done, aacc)
        done += 1
    per_a = aacc.shape[2]
    for p in range(aacc.shape[0]):
        prec[:, p * per_a : (p + 1) * per_a] = aacc[p].astype(BF16)
    kv[...] = prec[:, acols : acols + 2 * kcols]
    h_copies = []
    for at, step in ((0, 1), (1, n - 1)):
        made = pltpu.make_async_remote_copy(
            src_ref=kv,
            dst_ref=halo.at[at],
            send_sem=h_send.at[at],
            recv_sem=h_recv.at[at],
            device_id={"sp": lax.rem(me + step, n)},
        )
        made.start()
        h_copies.append(made)
    for made in h_copies:
        made.wait_recv()

    gap = (row - col).astype(F32)
    far_low, far_high = gap + rows, rows - gap
    ok_low = (far_low <= WINDOW) & (me > 0)
    ok_high = (far_high <= WINDOW) & (me < n - 1)
    bias = [
        jnp.where(ok_low, far_low, 1e30),
        jnp.where(jnp.abs(gap) <= WINDOW, jnp.abs(gap), 1e30),
        jnp.where(ok_high, far_high, 1e30),
    ]
    share = attn_heads // key_heads
    m_done = 0
    for h in range(attn_heads):
        at = (h // share) * HEAD
        q = prec[:, h * HEAD : (h + 1) * HEAD]
        slope = logits_ref[h : h + 1, 0:1]
        sink = logits_ref[h : h + 1, 1:2]
        parts = [halo.at[0], kv, halo.at[1]]
        keys = [part[:, at : at + HEAD] for part in parts]
        vals = [part[:, kcols + at : kcols + at + HEAD] for part in parts]
        scores = [
            dot(q, k, ((1,), (1,))) * HEAD ** (-0.5) - slope * b for k, b in zip(keys, bias)
        ]
        top = jnp.maximum(jnp.maximum(scores[0], scores[1]), scores[2])
        top = jnp.maximum(jnp.max(top, axis=-1, keepdims=True), sink)
        weights = [jnp.exp(s - top) for s in scores]
        total = jnp.sum(weights[0] + weights[1] + weights[2], axis=-1, keepdims=True)
        scale = 1.0 / (total + jnp.exp(sink - top))
        res = dot(weights[0], vals[0]) + dot(weights[1], vals[1]) + dot(weights[2], vals[2])
        feats[:, dcols + h * HEAD : dcols + (h + 1) * HEAD] = (res * scale).astype(BF16)
        while m_done < (n - 1) * (h + 1) // attn_heads:
            m_arrive(m_done, None)
            m_done += 1

    state[...] = start_ref[...]
    while m_done < n - 1:
        m_arrive(m_done, None)
        m_done += 1

    def apply(r, s):
        at = 0
        for size, stride in dims:
            mine_at, there = lax.rem(me // stride, size), lax.rem(s // stride, size)
            at = at + lax.rem(mine_at - there + size, size) * stride
        for h in range(heads):
            m = maps[h // half, at, r, h % half]
            now = state[r, h]
            high = now.astype(BF16)
            rest = (now - high.astype(F32)).astype(BF16)
            moved = dot(m[:, HEAD:], jnp.concatenate([high, rest], axis=1))
            state[r, h] = moved[:, :HEAD] + moved[:, HEAD:] + m[:, :HEAD].astype(F32)

    def forward_step(i, carry):
        apply(0, i)
        return carry

    def backward_step(i, carry):
        apply(1, n - 1 - i)
        return carry

    lax.fori_loop(0, me, forward_step, 0)
    lax.fori_loop(0, n - 1 - me, backward_step, 0)

    for h in range(heads):
        both = jnp.concatenate([state[0, h], state[1, h]], axis=0)
        y = base_out[h] + dot(reads[h], both)
        y = y * lax.rsqrt(jnp.mean(y * y, axis=-1, keepdims=True) + EPS) * norm_gain_ref[...]
        feats[:, h * HEAD : (h + 1) * HEAD] = y.astype(BF16)

    for made in w_copies:
        made.wait()
    step = min(512, width)
    each = rows // ntp
    for at in range(0, width, step):
        res = dot(feats[:, :dcols], wo[0, :, at : at + step]) + dot(
            feats[:, dcols:], wo[1, :, at : at + step]
        )
        res = res.astype(BF16)
        for p in range(ntp):
            partial[0, p, :, at : at + step] = res[p * each : (p + 1) * each]
    p_copies = []
    for k in range(1, ntp):
        peer = lax.rem(mt + k, ntp)
        made = pltpu.make_async_remote_copy(
            src_ref=partial.at[0, peer],
            dst_ref=partial.at[1, k],
            send_sem=p_send.at[k],
            recv_sem=p_recv.at[k],
            device_id={"tp": peer},
        )
        made.start()
        p_copies.append(made)
    total = partial[0, mt].astype(F32)
    for k in range(1, ntp):
        p_copies[k - 1].wait_recv()
        total = total + partial[1, k].astype(F32)
    out_ref[...] = total.astype(BF16)
    for made in h_copies + p_copies:
        made.wait_send()
    d_finish()
    a_finish()
    m_finish()


def cut(weights):
    joined = jnp.concatenate(weights, axis=1)
    rows, cols = joined.shape
    pieces = 4 if cols % 512 == 0 else 1
    return jnp.transpose(joined.reshape(rows, pieces, cols // pieces), (1, 0, 2))


def on_device(
    dims,
    tokens,
    input_norm_gain,
    delta_query_weight,
    delta_key_weight,
    delta_value_weight,
    gate_weight,
    head_decay_params,
    log_decay_increments,
    starting_state,
    delta_norm_gain,
    attention_query_weight,
    attention_key_weight,
    attention_value_weight,
    sink,
    delta_output_weight,
    attention_output_weight,
):
    n, ntp = lax.axis_size("sp"), lax.axis_size("tp")
    rows, width = tokens.shape
    heads = delta_query_weight.shape[1] // HEAD
    attn_heads = attention_query_weight.shape[1] // HEAD
    key_heads = attention_key_weight.shape[1] // HEAD
    gates = lax.dynamic_slice_in_dim(gate_weight, lax.axis_index("tp") * heads, heads, 2)
    gates = gates.reshape(gate_weight.shape[0], 4 * heads).T
    wd = [delta_query_weight, delta_key_weight, delta_value_weight]
    wa = [attention_query_weight, attention_key_weight, attention_value_weight]
    each = key_heads * HEAD
    if each % 128 == 0 and heads % key_heads == 0 and attn_heads % key_heads == 0:
        pd, pa = [sum(w.shape[1] for w in some) // each for some in (wd, wa)]
        shape_d = shape_a = (wd[0].shape[0], each)
    else:
        wd, wa = [cut(wd)], [cut(wa)]
        pd, pa, shape_d, shape_a = wd[0].shape[0], wa[0].shape[0], wd[0].shape[1:], wa[0].shape[1:]
    head_ids = (lax.axis_index("tp") * attn_heads + jnp.arange(attn_heads)).astype(F32)
    slopes = jnp.exp2(-8.0 * (head_ids + 1.0) / (attn_heads * ntp))
    logits = jnp.stack([slopes, sink], axis=1)
    cfg = (n, ntp, dims, heads, attn_heads, key_heads, len(wd), len(wa))
    dcols, acols, kcols = heads * HEAD, attn_heads * HEAD, key_heads * HEAD
    pm = 2 if heads % 2 == 0 else 1
    vmem = pl.BlockSpec(memory_space=pltpu.VMEM)
    hbm = pl.BlockSpec(memory_space=pl.ANY)
    dma = pltpu.SemaphoreType.DMA
    return pl.pallas_call(
        functools.partial(kernel, cfg),
        out_shape=jax.ShapeDtypeStruct((rows // ntp, width), BF16),
        in_specs=[vmem] * (8 + len(wd) + len(wa)) + [hbm] * 2,
        out_specs=vmem,
        scratch_shapes=[
            pltpu.VMEM((n, rows, width // n), BF16),
            pltpu.VMEM((pd, n) + shape_d, BF16),
            pltpu.VMEM((pa, n) + shape_a, BF16),
            pltpu.VMEM((pd, rows, shape_d[1]), F32),
            pltpu.VMEM((pa, rows, shape_a[1]), F32),
            pltpu.VMEM((rows, 3 * dcols), BF16),
            pltpu.VMEM((8, 128), BF16),
            pltpu.VMEM((rows, 2 * kcols), BF16),
            pltpu.VMEM((2, rows, 2 * kcols), BF16),
            pltpu.VMEM((pm, 2, heads // pm, HEAD, 2 * HEAD), BF16),
            pltpu.VMEM((pm, n, 2, heads // pm, HEAD, 2 * HEAD), BF16),
            pltpu.VMEM((2, heads, HEAD, HEAD), F32),
            pltpu.VMEM((heads, rows, HEAD), F32),
            pltpu.VMEM((heads, rows, 2 * HEAD), BF16),
            pltpu.VMEM((rows, dcols + acols), BF16),
            pltpu.VMEM((2,) + delta_output_weight.shape, BF16),
            pltpu.VMEM((2, ntp, rows // ntp, width), BF16),
            pltpu.VMEM((rows, acols + 2 * kcols), BF16),
            dma((pd, 2 * n)),
            dma((pd, n)),
            dma((pa, 2 * n)),
            dma((pa, n)),
            dma((pm, 2 * n)),
            dma((pm, n)),
            dma((2,)),
            dma((2,)),
            dma((ntp,)),
            dma((ntp,)),
            dma((2,)),
        ],
        compiler_params=pltpu.CompilerParams(
            collective_id=0, has_side_effects=True, vmem_limit_bytes=60 * 1024 * 1024
        ),
    )(
        tokens,
        input_norm_gain.reshape(1, -1),
        gates,
        head_decay_params.T,
        log_decay_increments,
        starting_state,
        delta_norm_gain.reshape(1, -1),
        logits,
        *wd,
        *wa,
        delta_output_weight,
        attention_output_weight,
    )


def solution(mesh):
    in_specs = (
        P("sp", None),
        P(),
        P("sp", "tp"),
        P("sp", "tp"),
        P("sp", "tp"),
        P(),
        P(None, "tp"),
        P("tp", "sp"),
        P(None, "tp", None, None),
        P(),
        P("sp", "tp"),
        P("sp", "tp"),
        P("sp", "tp"),
        P("tp"),
        P("tp", None),
        P("tp", None),
    )
    out_specs = P(("sp", "tp"), None)
    return jax.shard_map(
        functools.partial(on_device, ring_dims(mesh)),
        mesh=mesh,
        in_specs=in_specs,
        out_specs=out_specs,
        check_vma=False,
    )
```
